32 devices in a mesh: sp: 8 (over z, y), tp: 4 (over x, core).
Axes of the slice: x: 2, y: 2, z: 4, core: 2. Of those that a mesh axis runs over, the one named last changes fastest.
Arguments:
- tokens_in: bfloat16 [2048, 2048], P('sp'), may hold values from -3 to 3
- queries: bfloat16 [2048, 1024], P('sp', 'tp'), may hold values from -6 to 6
- keys: bfloat16 [2048, 256], P('sp', 'tp'), may hold values from -6 to 6
- values: bfloat16 [2048, 256], P('sp', 'tp'), may hold values from -12 to 12
- doc_ids: int32 [2048], P('sp'), may hold values from 0 to 1, never falling along the last dimension, each value on 1 to 1280 neighbouring positions
- query_gain: float32 [64], replicated, may hold values from 2.5 to 6
- key_norm_scale: float32 [64], replicated, may hold values from 2.5 to 6
- out_weight: bfloat16 [1024, 2048], P('tp'), may hold values from -0.1875 to 0.1875
- norm_gain: float32 [2048], replicated, may hold values from 0.1 to 1.9
- gate_weight: bfloat16 [2048, 5632], P('sp', 'tp'), may hold values from -0.125 to 0.125
- up_weight: bfloat16 [2048, 5632], P('sp', 'tp'), may hold values from -0.125 to 0.125
- down_weight: bfloat16 [5632, 2048], P('tp', 'sp'), may hold values from -0.078125 to 0.078125
Outputs:
- layer_out: bfloat16 [2048, 2048], P('sp')
The draws below stay inside these ranges and needn't reach their ends.
Inputs may be any that keep to these rules, and one draw needn't show every extreme that they name: `doc_ids`: document numbers never fall along the sequence; every document has 1 to 1280 positions and one has exactly 1280.
All inputs are finite; a program needn't handle non-finite values.
Results may differ from the reference program's by a relative error of at most 0.014.
The reference program's roundings to bfloat16 on the way (of `weights`, `attended`, `normed` and `hidden`) count: a program that leaves them out, or rounds other values in their place, can miss the bound.
Values may be sent and summed in bfloat16 or wider, within the bound.
No kernel may reach another device: no remote copies, remote signals or barrier semaphores. Data moves between devices by JAX's collectives and lax.ppermute only.
A program may use at most 128 MiB of HBM per device.

```python
import math
import jax
import jax.numpy as jnp
import numpy as np
from jax import lax

D = 2048
QUERY_HEADS = 16
KEY_VALUE_HEADS = 4
HEAD_SIZE = 64
FF = 5632
GRID = 64
PACKED_TOKENS = 2048
DOCS = 2
DOC_MOST = 1280
N_TP = 4


def repeated_keys(key):
    sampled_values = jax.random.normal(jax.random.fold_in(key, 11), (PACKED_TOKENS, KEY_VALUE_HEADS * HEAD_SIZE), jnp.float32)
    return jnp.clip(sampled_values, -6.0, 6.0)


def draw_keys(key, part):
    return repeated_keys(key).astype(jnp.bfloat16)


def draw_queries(key, part):
    fresh = jnp.clip(jax.random.normal(jax.random.fold_in(key, 12), (PACKED_TOKENS, QUERY_HEADS * HEAD_SIZE), jnp.float32), -6.0, 6.0)
    return fresh.astype(jnp.bfloat16)


def draw_query_gain(key, part):
    spread = jax.random.uniform(jax.random.fold_in(key, 21), (HEAD_SIZE,), jnp.float32)
    return 2.5 + spread


def draw_key_norm_scale(key, part):
    spread = jax.random.uniform(jax.random.fold_in(key, 22), (HEAD_SIZE,), jnp.float32)
    return 2.5 + spread


def shard_levels(own_key, extent, shards, least, largest):
    def one(dim, parts):
        heights = jax.random.uniform(jax.random.fold_in(jax.random.fold_in(own_key, 6), dim), (parts,), jnp.float32, least / len(shards), largest / len(shards))
        return jnp.repeat(jnp.exp(heights), extent[dim] // parts).reshape((-1,) + (1,) * (len(extent) - dim - 1))

    level = one(*shards[0])
    for cut in shards[1:]:
        level = level * one(*cut)
    return level


def split_up(amount, total, bound, skew):
    loads = [(1 << 20) // math.isqrt(rank ** skew) + 1 for rank in range(2, amount + 1)]
    surplus, counts = total - bound - (amount - 1), [1] * (amount - 1)
    while surplus > 0:
        movable = [i for i in range(amount - 1) if counts[i] < bound]
        mass, remaining = sum([loads[i] for i in movable]), surplus
        for i in movable:
            more = min(bound - counts[i], max(1, remaining * loads[i] // mass), surplus)
            counts[i] = counts[i] + more
            surplus = surplus - more
    return np.array([bound] + counts)


def ragged_sizes(stream_key, amount, total, limit, lean):
    if amount == 2:
        one = jax.random.randint(stream_key, (), max(1, total - limit), min(limit, total - 1) + 1)
        return jnp.stack([one, total - one])
    lengths = jnp.asarray(split_up(amount, total, limit, lean), jnp.int32)
    couples = (amount - 1) // 2
    giver, receiver = lengths[1:1 + 2 * couples:2], lengths[2:2 + 2 * couples:2]
    margin = jnp.minimum(giver - 1, limit - receiver)
    moved = jax.random.randint(jax.random.fold_in(stream_key, 1), (couples,), 0, 1 << 20) % (margin + 1)
    lengths = lengths.at[1:1 + 2 * couples:2].set(giver - moved).at[2:2 + 2 * couples:2].set(receiver + moved)
    return lengths[jax.random.permutation(jax.random.fold_in(stream_key, 2), amount)]


def scatter_about(own_key, dims, width, bound, shards=(), kind=jnp.bfloat16):
    level = shard_levels(own_key, dims, shards, -0.22, 0.18) if shards else 1.0
    drawn = jax.random.normal(own_key, dims, jnp.float32) * width * level
    return jnp.minimum(jnp.maximum(drawn, -bound), bound).astype(kind)


def setup_inputs(seed: int = 0) -> dict:
    key_list = jax.random.split(jax.random.key(seed), 13)
    return {
        "tokens_in": scatter_about(key_list[0], (PACKED_TOKENS, D), 0.5, 3.0, ((0, 8),)),
        "queries": draw_queries(jax.random.fold_in(key_list[12], 71), 0),
        "keys": draw_keys(jax.random.fold_in(key_list[12], 71), 0),
        "values": scatter_about(key_list[3], (PACKED_TOKENS, KEY_VALUE_HEADS * HEAD_SIZE), 2.0, 12.0, ((0, 8), (1, 4))),
        "doc_ids": jnp.searchsorted(jnp.cumsum(ragged_sizes(key_list[4], DOCS, PACKED_TOKENS, DOC_MOST, 1)), jnp.arange(PACKED_TOKENS), side="right").astype(jnp.int32),
        "query_gain": draw_query_gain(jax.random.fold_in(key_list[12], 71), 0),
        "key_norm_scale": draw_key_norm_scale(jax.random.fold_in(key_list[12], 71), 0),
        "out_weight": scatter_about(key_list[7], (QUERY_HEADS * HEAD_SIZE, D), (QUERY_HEADS * HEAD_SIZE) ** -0.5, 0.1875, ((0, 4),)),
        "norm_gain": jnp.clip(1.0 + 0.18 * jax.random.normal(key_list[8], (D,), jnp.float32), 0.1, 1.9),
        "gate_weight": scatter_about(key_list[9], (D, FF), D ** -0.5, 0.125, ((0, 8), (1, 4))),
        "up_weight": scatter_about(key_list[10], (D, FF), D ** -0.5, 0.125, ((0, 8), (1, 4))),
        "down_weight": scatter_about(key_list[11], (FF, D), FF ** -0.5, 0.078125, ((0, 4), (1, 8))),
    }


EPS = 1e-06
THETA = 10000.0
NEG = -1e+30

def rotate_half(block, angle):
    half_dim = block.shape[-1] // 2
    cosine = jnp.cos(angle)[:, None, :]
    sine = jnp.sin(angle)[:, None, :]
    first = block[..., :half_dim]
    second = block[..., half_dim:]
    return jnp.concatenate([first * cosine - second * sine, second * cosine + first * sine], axis=-1)

def normalized_rotated(values_in, gain, heads, lattice_row, lattice_column):
    full = values_in.astype(jnp.float32).reshape(values_in.shape[0], heads, -1)
    full = full * lax.rsqrt(lax.optimization_barrier(jnp.mean(full * full, axis=-1, keepdims=True)) + EPS) * gain
    half_dim = full.shape[-1] // 2
    freqs = THETA ** (-2.0 * jnp.arange(half_dim // 2, dtype=jnp.float32) / half_dim)
    by_row = rotate_half(full[..., :half_dim], lattice_row[:, None] * freqs[None, :])
    by_col = rotate_half(full[..., half_dim:], lattice_column[:, None] * freqs[None, :])
    return jnp.concatenate([by_row, by_col], axis=-1).astype(jnp.bfloat16)

def reference(tokens_in, queries, keys, values, doc_ids, query_gain, key_norm_scale, out_weight, norm_gain, gate_weight, up_weight, down_weight):
    places = jnp.arange(PACKED_TOKENS, dtype=jnp.int32)
    lattice_row = (places // GRID).astype(jnp.float32)
    lattice_column = (places % GRID).astype(jnp.float32)
    q_all = normalized_rotated(queries, query_gain, QUERY_HEADS, lattice_row, lattice_column)
    every_key = normalized_rotated(keys, key_norm_scale, KEY_VALUE_HEADS, lattice_row, lattice_column).astype(jnp.float32)
    every_value = values.reshape(PACKED_TOKENS, KEY_VALUE_HEADS, HEAD_SIZE).astype(jnp.float32)
    query_group = QUERY_HEADS // KEY_VALUE_HEADS
    scale = HEAD_SIZE ** (-0.5)
    rows_per_block = 128

    def attend(start):
        query_tile = lax.dynamic_slice_in_dim(q_all, start, rows_per_block, 0).astype(jnp.float32)
        query_tile = query_tile.reshape(rows_per_block, KEY_VALUE_HEADS, query_group, HEAD_SIZE)
        doc_block = lax.dynamic_slice_in_dim(doc_ids, start, rows_per_block, 0)
        scores = jnp.einsum('qhgd,khd->hgqk', query_tile, every_key) * scale
        same = (doc_block[:, None] == doc_ids[None, :])[None, None]
        scores = jnp.where(same, scores, NEG)
        top = lax.optimization_barrier(jnp.max(scores, axis=-1, keepdims=True))
        weights = jnp.where(same, jnp.exp(scores - top), 0.0)
        total = lax.optimization_barrier(jnp.sum(weights, axis=-1))
        rounded = lax.optimization_barrier(weights.astype(jnp.bfloat16)).astype(jnp.float32)
        blended = jnp.einsum('hgqk,khd->hgqd', rounded, every_value) / total[..., None]
        return blended.transpose(2, 0, 1, 3).reshape(rows_per_block, QUERY_HEADS * HEAD_SIZE).astype(jnp.bfloat16)
    starts = jnp.arange(PACKED_TOKENS // rows_per_block, dtype=jnp.int32) * rows_per_block
    attended = lax.map(attend, starts).reshape(PACKED_TOKENS, QUERY_HEADS * HEAD_SIZE)
    share_cols = QUERY_HEADS * HEAD_SIZE // N_TP
    mixed = jnp.zeros((PACKED_TOKENS, D), jnp.float32)
    for member in range(N_TP):
        part_out = jnp.dot(attended[:, member * share_cols:(member + 1) * share_cols], out_weight[member * share_cols:(member + 1) * share_cols], preferred_element_type=jnp.float32)
        mixed = mixed + part_out.astype(jnp.bfloat16).astype(jnp.float32)
    resid = tokens_in.astype(jnp.float32) + mixed
    normed = (resid * lax.rsqrt(lax.optimization_barrier(jnp.mean(resid * resid, axis=-1, keepdims=True)) + EPS) * norm_gain).astype(jnp.bfloat16)
    gate = jnp.dot(normed, gate_weight, preferred_element_type=jnp.float32)
    up_val = jnp.dot(normed, up_weight, preferred_element_type=jnp.float32)
    hidden = (jax.nn.silu(gate) * up_val).astype(jnp.bfloat16)
    unit_cols = FF // N_TP
    fed = jnp.zeros((PACKED_TOKENS, D), jnp.float32)
    for member in range(N_TP):
        part_out = jnp.dot(hidden[:, member * unit_cols:(member + 1) * unit_cols], down_weight[member * unit_cols:(member + 1) * unit_cols], preferred_element_type=jnp.float32)
        fed = fed + part_out.astype(jnp.bfloat16).astype(jnp.float32)
    return (resid + fed).astype(jnp.bfloat16)
```

```python
import functools

import jax
import jax.numpy as jnp
from jax import lax
from jax.experimental import pallas as pl
from jax.experimental.pallas import tpu as pltpu
from jax.sharding import PartitionSpec as P


GRID = 64


EPS = 1e-06
THETA = 10000.0
NEG = -1e30


def rotate_half(block, angle):
    half_dim = block.shape[-1] // 2
    cosine = jnp.cos(angle)[:, None, :]
    sine = jnp.sin(angle)[:, None, :]
    first = block[..., :half_dim]
    second = block[..., half_dim:]
    return jnp.concatenate(
        [first * cosine - second * sine, second * cosine + first * sine], axis=-1
    )


def normalized_rotated(values_in, gain, heads, lattice_row, lattice_column):
    full = values_in.astype(jnp.float32).reshape(values_in.shape[0], heads, -1)
    full = full * lax.rsqrt(jnp.mean(full * full, axis=-1, keepdims=True) + EPS) * gain
    half_dim = full.shape[-1] // 2
    freqs = THETA ** (-2.0 * jnp.arange(half_dim // 2, dtype=jnp.float32) / half_dim)
    by_row = rotate_half(full[..., :half_dim], lattice_row[:, None] * freqs[None, :])
    by_col = rotate_half(full[..., half_dim:], lattice_column[:, None] * freqs[None, :])
    return jnp.concatenate([by_row, by_col], axis=-1).astype(jnp.bfloat16)


def gathered_layer(
    tokens_in,
    queries,
    keys,
    values,
    doc_ids,
    query_gain,
    key_norm_scale,
    out_weight,
    norm_gain,
    gate_weight,
    up_weight,
    down_weight,
):
    tok_rows = tokens_in.shape[0]
    head_dim = query_gain.shape[0]
    local_heads = queries.shape[1] // head_dim
    places = lax.axis_index("sp") * tok_rows + jnp.arange(tok_rows, dtype=jnp.int32)
    lattice_row = (places // GRID).astype(jnp.float32)
    lattice_column = (places % GRID).astype(jnp.float32)
    q_local = normalized_rotated(queries, query_gain, local_heads, lattice_row, lattice_column)
    q_rows = q_local.transpose(1, 0, 2).reshape(local_heads * tok_rows, head_dim)
    key_pairs = normalized_rotated(keys, key_norm_scale, 1, lattice_row, lattice_column).reshape(
        tok_rows // 2, 2 * head_dim
    )
    value_pairs = values.reshape(tok_rows // 2, 2 * head_dim)
    doc_pairs = doc_ids.reshape(tok_rows // 2, 2)
    row_docs = jnp.tile(doc_ids, local_heads)
    first_doc = doc_ids[0]
    last_doc = doc_ids[-1]
    scale = head_dim ** (-0.5)
    total_rows = local_heads * tok_rows

    def absorb_block(state, key_block, value_block, doc_block):

        def absorb(current):
            running_max, running_sum, running_acc = current
            scores = (
                jnp.einsum("qd,kd->qk", q_rows, key_block, preferred_element_type=jnp.float32)
                * scale
            )
            same = row_docs[:, None] == doc_block[None, :]
            scores = jnp.where(same, scores, NEG)
            new_max = jnp.maximum(running_max, jnp.max(scores, axis=1))
            weights = jnp.where(same, jnp.exp(scores - new_max[:, None]), 0.0)
            shrink = jnp.exp(running_max - new_max)
            new_sum = running_sum * shrink + jnp.sum(weights, axis=1)
            new_acc = running_acc * shrink[:, None] + jnp.dot(
                weights.astype(jnp.bfloat16), value_block, preferred_element_type=jnp.float32
            )
            return (new_max, new_sum, new_acc)

        touches = (doc_block[0] <= last_doc) & (doc_block[-1] >= first_doc)
        return lax.cond(touches, absorb, lambda current: current, state)

    initial = (
        jnp.full((total_rows,), NEG, jnp.float32),
        jnp.zeros((total_rows,), jnp.float32),
        jnp.zeros((total_rows, head_dim), jnp.float32),
    )
    carry = initial
    key_piece = lax.all_gather(key_pairs, "sp", axis=0, tiled=True)
    value_piece = lax.all_gather(value_pairs, "sp", axis=0, tiled=True)
    doc_piece = lax.all_gather(doc_pairs, "sp", axis=0, tiled=True)
    shards = key_piece.shape[0] * 2 // tok_rows
    joined = 1
    while joined * 2 <= shards and shards % (joined * 2) == 0 and (joined * 2 * tok_rows <= 1024):
        joined = joined * 2
    blocks = shards // joined
    span_rows = joined * tok_rows
    key_blocks = key_piece.reshape(blocks, span_rows, head_dim)
    value_blocks = value_piece.reshape(blocks, span_rows, head_dim)
    doc_blocks = doc_piece.reshape(blocks, span_rows)

    def visit(state, inputs):
        key_block, value_block, doc_block = inputs
        return (absorb_block(state, key_block, value_block, doc_block), None)

    carry, unused = lax.scan(visit, carry, (key_blocks, value_blocks, doc_blocks))
    attended = (carry[2] / carry[1][:, None]).astype(jnp.bfloat16)
    attended = (
        attended.reshape(local_heads, tok_rows, head_dim)
        .transpose(1, 0, 2)
        .reshape(tok_rows, local_heads * head_dim)
    )
    partial_value = jnp.dot(attended, out_weight, preferred_element_type=jnp.float32)
    mixed = lax.psum(
        partial_value.astype(jnp.bfloat16).astype(jnp.float32).astype(jnp.bfloat16), "tp"
    ).astype(jnp.float32)
    resid = tokens_in.astype(jnp.float32) + mixed
    normed = (
        resid * lax.rsqrt(jnp.mean(resid * resid, axis=-1, keepdims=True) + EPS) * norm_gain
    ).astype(jnp.bfloat16)
    gate = jnp.dot(
        normed,
        lax.all_gather(gate_weight, "sp", axis=0, tiled=True),
        preferred_element_type=jnp.float32,
    )
    up_val = jnp.dot(
        normed,
        lax.all_gather(up_weight, "sp", axis=0, tiled=True),
        preferred_element_type=jnp.float32,
    )
    hidden = (jax.nn.silu(gate) * up_val).astype(jnp.bfloat16)
    fed_part = jnp.dot(
        hidden,
        lax.all_gather(down_weight, "sp", axis=1, tiled=True),
        preferred_element_type=jnp.float32,
    )
    fed = lax.psum(
        fed_part.astype(jnp.bfloat16).astype(jnp.float32).astype(jnp.bfloat16), "tp"
    ).astype(jnp.float32)
    return (resid + fed).astype(jnp.bfloat16)


LANES = 128
AXES = ("sp", "tp")
MB = 1 << 20


def swap(value, planes, sides, members, flip):
    dz, dy, dt = flip
    pairs = []
    for z in range(planes):
        for y in range(sides):
            for t in range(members):
                here = (z * sides + y) * members + t
                there = ((z ^ dz) * sides + (y ^ dy)) * members + (t ^ dt)
                pairs.append((here, there))
    return lax.ppermute(value, AXES, pairs)


def after(value, *others):
    return lax.optimization_barrier((value, *others))[0]


def attend_kernel(heads, quarters, index, q_ref, doc_ref, w_ref, *refs):
    pieces, outs = refs[:-quarters], refs[-quarters:]
    rows, head_dim = q_ref.shape[0], q_ref.shape[1] // heads
    keys = jnp.concatenate([p[:rows, :head_dim] for p in pieces], axis=0)
    values = jnp.concatenate([p[:rows, head_dim:] for p in pieces], axis=0)
    docs = []
    for p in pieces:
        tail = p[rows:, :].astype(jnp.float32)
        docs += [tail[i : i + 1, :] for i in range(rows // LANES)]
    same = doc_ref[...] == jnp.concatenate(docs, axis=1)
    attended = []
    for h in range(heads):
        q = q_ref[:, h * head_dim : (h + 1) * head_dim]
        scores = lax.dot_general(q, keys, (((1,), (1,)), ((), ())), preferred_element_type=jnp.float32)
        scores = jnp.where(same, scores * head_dim ** (-0.5), NEG)
        top = jnp.max(scores, axis=1, keepdims=True)
        weights = jnp.where(same, jnp.exp(scores - top), 0.0)
        total = jnp.sum(weights, axis=1, keepdims=True)
        blended = jnp.dot(weights.astype(jnp.bfloat16), values, preferred_element_type=jnp.float32)
        attended.append((blended / total).astype(jnp.bfloat16))
    attended = jnp.concatenate(attended, axis=1)
    mixed = jnp.dot(attended, w_ref[...], preferred_element_type=jnp.float32).astype(jnp.bfloat16)
    part = rows // quarters
    for member in range(quarters):
        for flip in range(quarters):

            @pl.when((index[0] ^ flip) == member)
            def _():
                outs[flip][...] = mixed[member * part : (member + 1) * part, :]


def attend(q, doc_column, out_weight, pieces, member, heads, quarters):
    rows, width = q.shape[0], out_weight.shape[1]
    vmem = pl.BlockSpec(memory_space=pltpu.VMEM)
    return pl.pallas_call(
        functools.partial(attend_kernel, heads, quarters),
        out_shape=[jax.ShapeDtypeStruct((rows // quarters, width), jnp.bfloat16)] * quarters,
        in_specs=[pl.BlockSpec(memory_space=pltpu.SMEM)] + [vmem] * (3 + len(pieces)),
        out_specs=[vmem] * quarters,
        compiler_params=pltpu.CompilerParams(vmem_limit_bytes=48 * MB),
        name="attend",
    )(member, q, doc_column, out_weight, *pieces)


def hidden_kernel(groups, blocks, index, *refs):
    n_tok, n_w = groups, 2 * blocks
    tokens, weights = refs[:n_tok], refs[n_tok : n_tok + n_w]
    out, held, sems = refs[n_tok + n_w :]
    copies = []
    for i, w in enumerate(weights):
        copies.append(pltpu.make_async_copy(w, held.at[i], sems.at[i]))
        copies[-1].start()
    part = tokens[0].shape[0]
    depth, width = held.shape[1] // 2, held.shape[2]
    gates, ups = [None, None], [None, None]
    for k in range(blocks):
        at = pl.ds(pl.multiple_of((index[0] ^ k) * depth, depth), depth)
        x = jnp.concatenate([t[:, at] for t in tokens], axis=0)
        for c in range(2):
            copies[2 * k + c].wait()
            g = jnp.dot(x, held[2 * k + c, :depth, :], preferred_element_type=jnp.float32)
            u = jnp.dot(x, held[2 * k + c, depth:, :], preferred_element_type=jnp.float32)
            gates[c] = g if gates[c] is None else gates[c] + g
            ups[c] = u if ups[c] is None else ups[c] + u
    lane = lax.broadcasted_iota(jnp.int32, (part * n_tok, width), 1)
    for c in range(2):
        gate, up = gates[c], ups[c]
        value = gate / (1.0 + jnp.exp(-gate)) * up
        value = jnp.where(lane >= index[1], value, 0.0)
        out[:, c * width : (c + 1) * width] = value.astype(jnp.bfloat16)


def hidden_units(tokens, weights, index):
    groups, blocks = len(tokens), len(weights) // 2
    vmem = pl.BlockSpec(memory_space=pltpu.VMEM)
    rows = sum(t.shape[0] for t in tokens)
    width = weights[0].shape[1]
    return pl.pallas_call(
        functools.partial(hidden_kernel, groups, blocks),
        out_shape=jax.ShapeDtypeStruct((rows, 2 * width), jnp.bfloat16),
        in_specs=[pl.BlockSpec(memory_space=pltpu.SMEM)] + [vmem] * groups + [pl.BlockSpec(memory_space=pl.ANY)] * len(weights),
        out_specs=vmem,
        scratch_shapes=[
            pltpu.VMEM((len(weights),) + weights[0].shape, jnp.bfloat16),
            pltpu.SemaphoreType.DMA((len(weights),)),
        ],
        compiler_params=pltpu.CompilerParams(vmem_limit_bytes=48 * MB),
        name="hidden",
    )(index, *tokens, *weights)


def down_kernel(groups, blocks, index, hidden_ref, *refs):
    weights, outs = refs[: 2 * blocks], refs[2 * blocks : 2 * blocks + groups]
    held, sems = refs[2 * blocks + groups :]
    copies = []
    for i, w in enumerate(weights):
        copies.append(pltpu.make_async_copy(w, held.at[i], sems.at[i]))
        copies[-1].start()
    part = outs[0].shape[0]
    depth, width = held.shape[1], held.shape[2]
    for k in range(blocks):
        at = pl.ds(pl.multiple_of((index[0] ^ k) * width, width), width)
        total = None
        for c in range(2):
            copies[2 * k + c].wait()
            piece = jnp.dot(
                hidden_ref[:, c * depth : (c + 1) * depth], held[2 * k + c], preferred_element_type=jnp.float32
            )
            total = piece if total is None else total + piece
        for g in range(groups):
            outs[g][:, at] = total[g * part : (g + 1) * part, :].astype(jnp.bfloat16)


def down_parts(hidden, weights, index, groups):
    blocks = len(weights) // 2
    vmem = pl.BlockSpec(memory_space=pltpu.VMEM)
    part = hidden.shape[0] // groups
    width = weights[0].shape[1] * blocks
    return pl.pallas_call(
        functools.partial(down_kernel, groups, blocks),
        out_shape=[jax.ShapeDtypeStruct((part, width), jnp.bfloat16)] * groups,
        in_specs=[pl.BlockSpec(memory_space=pltpu.SMEM), vmem] + [pl.BlockSpec(memory_space=pl.ANY)] * len(weights),
        out_specs=[vmem] * groups,
        scratch_shapes=[
            pltpu.VMEM((len(weights),) + weights[0].shape, jnp.bfloat16),
            pltpu.SemaphoreType.DMA((len(weights),)),
        ],
        compiler_params=pltpu.CompilerParams(vmem_limit_bytes=48 * MB),
        name="down",
    )(index, hidden, *weights)


def exchanged_layer(
    planes,
    sides,
    members,
    tokens_in,
    queries,
    keys,
    values,
    doc_ids,
    query_gain,
    key_norm_scale,
    out_weight,
    norm_gain,
    gate_weight,
    up_weight,
    down_weight,
):
    send = functools.partial(swap, planes=planes, sides=sides, members=members)
    tok_rows = tokens_in.shape[0]
    head_dim = query_gain.shape[0]
    heads = queries.shape[1] // head_dim
    place, member = lax.axis_index("sp"), lax.axis_index("tp")
    plane = place // sides
    part = tok_rows // members

    places = place * tok_rows + jnp.arange(tok_rows, dtype=jnp.int32)
    lattice_row = (places // GRID).astype(jnp.float32)
    lattice_column = (places % GRID).astype(jnp.float32)
    k_local = normalized_rotated(keys, key_norm_scale, 1, lattice_row, lattice_column).reshape(tok_rows, head_dim)
    doc_rows = doc_ids.astype(jnp.bfloat16).reshape(tok_rows // LANES, LANES)
    doc_rows = jnp.pad(doc_rows, ((0, 16 - doc_rows.shape[0]), (0, 0)))
    payload = jnp.concatenate([jnp.concatenate([k_local, values], axis=1), doc_rows], axis=0)
    kv_z = [payload] + [send(payload, flip=(dz, 0, 0)) for dz in range(1, planes)]
    kv = kv_z + [send(p, flip=(0, 1, 0)) for p in kv_z]

    hidden = gate_weight.shape[1]
    width = -(-(hidden // LANES) // planes) * LANES
    start_of = lambda z: jnp.minimum(z * width, hidden - width)
    stage = None
    both, downs = [], []
    for dz in range(planes):
        at = start_of(plane ^ dz)
        both.append(
            jnp.concatenate(
                [lax.dynamic_slice_in_dim(gate_weight, at, width, 1), lax.dynamic_slice_in_dim(up_weight, at, width, 1)],
                axis=0,
            )
        )
        downs.append(lax.dynamic_slice_in_dim(down_weight, at, width, 0))
    order = [2, 3, 1]
    gate_up, down = {0: both[0]}, {0: downs[0]}
    last = None
    for store, source in ((gate_up, both), (down, downs)):
        for dz in order:
            operand = source[dz] if last is None else after(source[dz], last)
            last = send(operand, flip=(dz, 0, 0))
            store[dz] = last
    gu_pieces, dn_pieces = [], []
    for store, pieces in ((gate_up, gu_pieces), (down, dn_pieces)):
        for dz in range(planes):
            own = store[dz]
            other = send(own, flip=(0, 1, 0))
            pieces += [own, send(own, flip=(0, 0, 1)), other, send(other, flip=(0, 0, 1))]

    q_local = normalized_rotated(queries, query_gain, heads, lattice_row, lattice_column).reshape(tok_rows, -1)
    mixed = attend(
        q_local, doc_ids.astype(jnp.float32).reshape(tok_rows, 1), out_weight, kv, member.reshape(1), heads, members
    )
    total = mixed[0].astype(jnp.float32)
    for dt in range(1, members):
        total = total + send(mixed[dt], flip=(0, 0, dt)).astype(jnp.float32)
    resid = lax.dynamic_slice_in_dim(tokens_in, member * part, part, 0).astype(jnp.float32) + total
    normed = (
        resid * lax.rsqrt(jnp.mean(resid * resid, axis=-1, keepdims=True) + EPS) * norm_gain
    ).astype(jnp.bfloat16)

    near = [normed] + [send(normed, flip=(dz, 0, 0)) for dz in range(1, planes)]
    far = [send(n, flip=(0, 0, 2)) for n in near]
    index = jnp.stack([place, plane * width - start_of(plane)]).astype(jnp.int32)
    units = hidden_units(near + far, gu_pieces, index)
    parts = down_parts(units, dn_pieces, index, 2 * planes)
    own, other = parts[:planes], parts[planes:]
    fed = None
    for dz in (3, 2, 1, 0):
        pair = own[dz].astype(jnp.float32) + send(other[dz], flip=(0, 0, 2)).astype(jnp.float32)
        if dz:
            pair = send(pair.astype(jnp.bfloat16), flip=(dz, 0, 0)).astype(jnp.float32)
        fed = pair if fed is None else fed + pair
    out = (resid + fed).astype(jnp.bfloat16)
    out_x = send(out, flip=(0, 0, 2))
    flips = [out, send(out, flip=(0, 0, 1)), out_x, send(out_x, flip=(0, 0, 1))]
    layer_out = jnp.zeros((tok_rows, tokens_in.shape[1]), jnp.bfloat16)
    for dt in range(members):
        layer_out = lax.dynamic_update_slice_in_dim(layer_out, flips[dt], (member ^ dt) * part, 0)
    return layer_out


def solution(mesh):
    members = mesh.shape["tp"]
    sides = mesh.shape["sp"] // members
    if sides == 2 and members == 4:
        layer = functools.partial(exchanged_layer, members, sides, members)
    else:
        layer = gathered_layer
    return jax.shard_map(
        layer,
        mesh=mesh,
        in_specs=(
            P("sp", None),
            P("sp", "tp"),
            P("sp", "tp"),
            P("sp", "tp"),
            P("sp"),
            P(),
            P(),
            P("tp", None),
            P(),
            P("sp", "tp"),
            P("sp", "tp"),
            P("tp", "sp"),
        ),
        out_specs=P("sp", None),
        check_vma=False,
    )
```
